32 devices in a mesh: ra: 8 (over z, y), cb: 4 (over x, core).
Axes of the slice: x: 2, y: 2, z: 4, core: 2. Of those that a mesh axis runs over, the one named last changes fastest.
Arguments:
- tokens: bfloat16 [128, 2048], P(None, 'ra'), may hold values from -6 to 6
- pre_gain: float32 [2, 2048], P(None, 'ra'), may hold values from 0.1 to 1.9
- post_gain: float32 [2, 2048], P(None, 'ra'), may hold values from 0.1 to 1.9
- gate_weight: bfloat16 [2, 2048, 5632], P(None, 'ra', 'cb'), may hold values from -0.125 to 0.125
- up_weight: bfloat16 [2, 2048, 5632], P(None, 'ra', 'cb'), may hold values from -0.125 to 0.125
- down_weight: bfloat16 [2, 5632, 2048], P(None, 'cb', 'ra'), may hold values from -0.078125 to 0.078125
Outputs:
- mixed: bfloat16 [128, 2048], P(None, 'ra')
The draws below stay inside these ranges and needn't reach their ends.
All inputs are finite; a program needn't handle non-finite values.
Results may differ from the reference program's by a relative error of at most 0.008.
Values may be sent and summed in bfloat16 or wider, within the bound.
A program may use at most 64 MiB of HBM per device.

```python
import jax
import jax.numpy as jnp
from jax import lax

D = 2048
FF = 5632
LAYERS = 2
TOKENS = 128


def with_spikes(result, key, source, target, parts, factor):
    owner, partner = [(jnp.arange(result.shape[position]) // (result.shape[position] // parts)).reshape([-1 if axis == position else 1 for axis in range(result.ndim)]) for position in (source, target)]
    chosen = jax.random.permutation(key, parts)[partner]
    strong = (owner == chosen) | (owner == (partner + parts // 2) % parts)
    return jnp.where(strong, factor * result, result)


def level_of(stream_key, extent, shards, low, high):
    gain, own = 1.0, jax.random.fold_in(stream_key, 6)
    for position, parts in shards:
        draws = jnp.exp(jax.random.uniform(jax.random.fold_in(own, position), (parts,), jnp.float32, low / len(shards), high / len(shards)))
        gain = gain * jnp.repeat(draws, extent[position] // parts).reshape([-1 if axis == position else 1 for axis in range(len(extent))])
    return gain


def bell_draw(key, extent, spread, most, shards=(), held_as=jnp.bfloat16):
    loudness = level_of(key, extent, shards, -0.22, 0.18) if shards else 1.0
    result = jax.random.normal(key, extent, jnp.float32) * spread * loudness
    return jnp.minimum(jnp.maximum(result, -most), most).astype(held_as)


def heavy_noise(stream_key, extent, deviation, reach, cuts, heavy, kind=jnp.bfloat16):
    values = deviation * jax.random.normal(stream_key, extent, jnp.float32)
    if cuts:
        values = values * level_of(stream_key, extent, cuts, -0.22, 0.18)
    return jnp.clip(with_spikes(values, jax.random.fold_in(stream_key, 3), *heavy), -reach, reach).astype(kind)


def setup_inputs(seed: int = 0) -> dict:
    key_list = jax.random.split(jax.random.key(seed), 7)
    tokens = heavy_noise(key_list[0], (TOKENS, D), 1.0, 6.0, ((1, 8),), (1, 0, 8, 2.0))
    pre_gain = jnp.clip(1.0 + 0.18 * jax.random.normal(key_list[1], (LAYERS, D), jnp.float32), 0.1, 1.9)
    post_gain = jnp.clip(1.0 + 0.18 * jax.random.normal(key_list[2], (LAYERS, D), jnp.float32), 0.1, 1.9)
    gate_weight = bell_draw(key_list[3], (LAYERS, D, FF), D ** -0.5, 0.125, ((1, 8), (2, 4)))
    up_weight = bell_draw(key_list[4], (LAYERS, D, FF), D ** -0.5, 0.125, ((1, 8), (2, 4)))
    down_weight = bell_draw(key_list[5], (LAYERS, FF, D), FF ** -0.5, 0.078125, ((1, 4), (2, 8)))
    return {"tokens": tokens, "pre_gain": pre_gain, "post_gain": post_gain, "gate_weight": gate_weight, "up_weight": up_weight, "down_weight": down_weight}


epsilon = 1e-06
residual_scale = 0.25

def reference(tokens, pre_gain, post_gain, gate_weight, up_weight, down_weight):
    stream = tokens.astype(jnp.float32)
    for sublayer in range(LAYERS):
        scale_in = lax.rsqrt(lax.optimization_barrier(jnp.mean(stream * stream, axis=1, keepdims=True)) + epsilon)
        normed = (stream * scale_in * pre_gain[sublayer]).astype(jnp.bfloat16)
        gate_sum = jnp.dot(normed, gate_weight[sublayer], preferred_element_type=jnp.float32)
        up_sum = jnp.dot(normed, up_weight[sublayer], preferred_element_type=jnp.float32)
        hidden = (jax.nn.silu(gate_sum) * up_sum).astype(jnp.bfloat16)
        branch = jnp.dot(hidden, down_weight[sublayer], preferred_element_type=jnp.float32)
        scale_out = lax.rsqrt(lax.optimization_barrier(jnp.mean(branch * branch, axis=1, keepdims=True)) + epsilon)
        stream = residual_scale * stream + branch * scale_out * post_gain[sublayer]
    return stream.astype(jnp.bfloat16)
```

```python
import functools

import jax
import jax.numpy as jnp
from jax import lax
from jax.experimental import pallas as pl
from jax.experimental.pallas import tpu as pltpu
from jax.sharding import PartitionSpec as P

EPS = 1e-06
RES = 0.25
LANES = 128
CHUNKS = 4
F32 = jnp.float32
BF16 = jnp.bfloat16


def plain_body(width, tokens, pre_gain, post_gain, gate_weight, up_weight, down_weight):
    stream = tokens.astype(F32)
    squares = lax.psum(jnp.sum(stream * stream, axis=1), "ra")
    for l in range(pre_gain.shape[0]):
        scale_in = lax.rsqrt(squares / width + EPS)
        normed = (stream * scale_in[:, None] * pre_gain[l]).astype(BF16)
        gate = jnp.dot(normed, gate_weight[l], preferred_element_type=F32)
        up = jnp.dot(normed, up_weight[l], preferred_element_type=F32)
        gate, up = lax.psum((gate, up), "ra")
        hidden = (jax.nn.silu(gate) * up).astype(BF16)
        branch = lax.psum(jnp.dot(hidden, down_weight[l], preferred_element_type=F32), "cb")
        gained = branch * post_gain[l]
        b_sq, g_sq, cross = lax.psum(
            (
                jnp.sum(branch * branch, axis=1),
                jnp.sum(gained * gained, axis=1),
                jnp.sum(stream * gained, axis=1),
            ),
            "ra",
        )
        scale_out = lax.rsqrt(b_sq / width + EPS)
        squares = RES * RES * squares + 2.0 * RES * scale_out * cross + scale_out * scale_out * g_sq
        stream = RES * stream + gained * scale_out[:, None]
    return stream.astype(BF16)


def kernel(
    R, Y, C, groups, width,
    tok, pre, post, gw_h, uw_h, dw_h, out,
    gw, uw, dw, normed, sq, st_s, st_r, y_s, y_r, own, z_s, z_r, hall, b_p, b_r, fin,
    w_sem, st_ss, st_rs, y_ss, y_rs, z_ss, z_rs, hz_ss, hz_rs, hy_ss, hy_rs, b_ss, b_rs, n_ss, n_rs,
):
    Z = R // Y
    L = pre.shape[0]
    T = tok.shape[0]
    G = len(groups)
    tz = T // R
    ty = T // Y
    tc = T // C
    per = ty // tc
    ra = lax.axis_index("ra")
    c = lax.axis_index("cb")
    z = ra // Y
    y = lax.rem(ra, Y)

    loads = []
    for l in range(L):
        for k, (src, dst) in enumerate(((gw_h, gw), (uw_h, uw), (dw_h, dw))):
            cp = pltpu.make_async_copy(src.at[l], dst.at[l], w_sem.at[l, k])
            cp.start()
            loads.append(cp)

    bar = pltpu.get_barrier_semaphore()
    for s in range(1, R):
        pl.semaphore_signal(bar, inc=1, device_id={"ra": lax.rem(ra + s, R)}, device_id_type=pl.DeviceIdType.MESH)
    for s in range(1, C):
        pl.semaphore_signal(bar, inc=1, device_id={"cb": lax.rem(c + s, C)}, device_id_type=pl.DeviceIdType.MESH)

    sends = []

    def push(src, dst, ss, rs, axis, where):
        cp = pltpu.make_async_remote_copy(
            src_ref=src, dst_ref=dst, send_sem=ss, recv_sem=rs,
            device_id={axis: where}, device_id_type=pl.DeviceIdType.MESH,
        )
        cp.start()
        sends.append(cp)
        return cp

    def z_at(s):
        return lax.rem(z + s, Z) * Y + y

    def y_at(s):
        return z * Y + lax.rem(y + s, Y)

    def share_stats(i, columns):
        rows = columns[0].shape[0]
        lane = lax.broadcasted_iota(jnp.int32, (rows, LANES), 1)
        packed = jnp.zeros((rows, LANES), F32)
        for k, col in enumerate(columns):
            packed = jnp.where(lane == k, col, packed)
        if rows < LANES:
            packed = jnp.concatenate([packed, jnp.zeros((LANES - rows, LANES), F32)], axis=0)
        st_s[i] = packed.T[:8]
        cps = [
            push(st_s.at[i], st_r.at[i, s - 1], st_ss.at[i, s - 1], st_rs.at[i, s - 1], "ra", lax.rem(ra + s, R))
            for s in range(1, R)
        ]
        total = st_s[i]
        for s, cp in enumerate(cps):
            cp.wait_recv()
            total = total + st_r[i, s]
        turned = jnp.concatenate([total, jnp.zeros((LANES - 8, LANES), F32)], axis=0).T
        return [turned[:rows, k : k + 1] for k in range(len(columns))]

    tokens = tok[...].astype(F32)
    local_sq = jnp.sum(tokens * tokens, axis=1, keepdims=True)
    pl.semaphore_wait(bar, R + C - 2)

    (squares_all,) = share_stats(0, [local_sq])
    sq[...] = jnp.broadcast_to(squares_all, (T, LANES)).reshape(C, tc, LANES)
    first = (tokens * lax.rsqrt(squares_all / width + EPS) * pre[0:1, :]).astype(BF16)
    normed[0] = first.reshape(C, tc, first.shape[1])

    squares = sq[c][:, 0:1]
    stream = tok[pl.ds(pl.multiple_of(c * tc, tc), tc), :].astype(F32)

    for l in range(L):
        loads[3 * l].wait()
        loads[3 * l + 1].wait()

        def partial(half, b0, nb):
            rows = normed[l, pl.ds(half * per, per)].reshape(ty, normed.shape[-1])
            cols = slice(b0 * LANES, (b0 + nb) * LANES)
            return (
                jnp.dot(rows, gw[l, :, cols], preferred_element_type=F32),
                jnp.dot(rows, uw[l, :, cols], preferred_element_type=F32),
            )

        y_cp, z_cp, hz_cp, hy_cp = {}, {}, {}, {}

        def stage_a(g):
            b0, nb = groups[g]
            for s in range(1, Y):
                ga, ua = partial(lax.rem(y + s, Y), b0, nb)
                for i in range(nb):
                    y_s[l, s - 1, b0 + i, :, :LANES] = ga[:, i * LANES : (i + 1) * LANES].astype(BF16)
                    y_s[l, s - 1, b0 + i, :, LANES:] = ua[:, i * LANES : (i + 1) * LANES].astype(BF16)
                y_cp[g, s] = push(
                    y_s.at[l, s - 1, pl.ds(b0, nb)], y_r.at[l, s - 1, pl.ds(b0, nb)],
                    y_ss.at[l, g, s - 1], y_rs.at[l, g, s - 1], "ra", y_at(s),
                )

        def stage_a2(g):
            b0, nb = groups[g]
            ga, ua = partial(y, b0, nb)
            for i in range(nb):
                own[b0 + i, :, :LANES] = ga[:, i * LANES : (i + 1) * LANES]
                own[b0 + i, :, LANES:] = ua[:, i * LANES : (i + 1) * LANES]

        def stage_b(g):
            b0, nb = groups[g]
            total = own[b0 : b0 + nb]
            for s in range(1, Y):
                y_cp[g, s].wait_recv()
                total = total + y_r[l, s - 1, b0 : b0 + nb].astype(F32)
            own[b0 : b0 + nb] = total
            low = total.astype(BF16)
            for q in range(Z):
                z_s[l, q, b0 : b0 + nb] = low[:, q * tz : (q + 1) * tz, :]
            for s in range(1, Z):
                z_cp[g, s] = push(
                    z_s.at[l, lax.rem(z + s, Z), pl.ds(b0, nb)], z_r.at[l, s - 1, pl.ds(b0, nb)],
                    z_ss.at[l, g, s - 1], z_rs.at[l, g, s - 1], "ra", z_at(s),
                )

        def stage_c(g):
            b0, nb = groups[g]
            total = own[b0 : b0 + nb, pl.ds(pl.multiple_of(z * tz, tz), tz), :]
            for s in range(1, Z):
                z_cp[g, s].wait_recv()
                total = total + z_r[l, s - 1, b0 : b0 + nb].astype(F32)
            gate, up = total[:, :, :LANES], total[:, :, LANES:]
            hall[l, y, z, b0 : b0 + nb] = (gate / (1.0 + jnp.exp(-gate)) * up).astype(BF16)
            mine = hall.at[l, y, z, pl.ds(b0, nb)]
            for s in range(1, Z):
                hz_cp[g, s] = push(mine, mine, hz_ss.at[l, g, s - 1], hz_rs.at[l, g, s - 1], "ra", z_at(s))
            for s in range(1, Y):
                hy_cp[g, 0, s] = push(mine, mine, hy_ss.at[l, g, 0, s - 1], hy_rs.at[l, g, 0, s - 1], "ra", y_at(s))

        def stage_d(g):
            b0, nb = groups[g]
            for r in range(1, Z):
                hz_cp[g, r].wait_recv()
                got = hall.at[l, y, lax.rem(z + Z - r, Z), pl.ds(b0, nb)]
                for s in range(1, Y):
                    hy_cp[g, r, s] = push(got, got, hy_ss.at[l, g, r, s - 1], hy_rs.at[l, g, r, s - 1], "ra", y_at(s))

        def stage_e(g, acc):
            b0, nb = groups[g]
            for r in range(Z):
                for s in range(1, Y):
                    hy_cp[g, r, s].wait_recv()
            lhs = jnp.concatenate([hall[l, :, :, b0 + i].reshape(T, LANES) for i in range(nb)], axis=1)
            part = jnp.dot(lhs, dw[l, b0 * LANES : (b0 + nb) * LANES, :], preferred_element_type=F32)
            return part if acc is None else acc + part

        for g in range(G):
            stage_a(g)
        for g in range(G):
            stage_a2(g)
        acc = None
        for t in range(G + 3):
            if t < G:
                stage_b(t)
            if 0 <= t - 1 < G:
                stage_c(t - 1)
            if 0 <= t - 2 < G:
                stage_d(t - 2)
            if 0 <= t - 3 < G:
                if t == 3:
                    loads[3 * l + 2].wait()
                acc = stage_e(t - 3, acc)

        b_p[l] = acc.reshape(C, tc, acc.shape[1])
        cps = []
        for s in range(1, C):
            to = lax.rem(c + s, C)
            cps.append(push(b_p.at[l, to], b_r.at[l, s - 1], b_ss.at[l, s - 1], b_rs.at[l, s - 1], "cb", to))
        branch = b_p[l, c]
        for s, cp in enumerate(cps):
            cp.wait_recv()
            branch = branch + b_r[l, s]

        gained = branch * post[l : l + 1, :]
        b_sq, g_sq, cross = share_stats(
            l + 1,
            [
                jnp.sum(branch * branch, axis=1, keepdims=True),
                jnp.sum(gained * gained, axis=1, keepdims=True),
                jnp.sum(stream * gained, axis=1, keepdims=True),
            ],
        )
        scale_out = lax.rsqrt(b_sq / width + EPS)
        squares = RES * RES * squares + 2.0 * RES * scale_out * cross + scale_out * scale_out * g_sq
        stream = RES * stream + gained * scale_out
        if l + 1 < L:
            scale_in = lax.rsqrt(squares / width + EPS)
            normed[l + 1, c] = (stream * scale_in * pre[l + 1 : l + 2, :]).astype(BF16)
            mine = normed.at[l + 1, c]
        else:
            fin[c] = stream.astype(BF16)
            mine = fin.at[c]
        cps = [
            push(mine, mine, n_ss.at[l, s - 1], n_rs.at[l, s - 1], "cb", lax.rem(c + s, C))
            for s in range(1, C)
        ]
        for cp in cps:
            cp.wait_recv()

    out[...] = fin[...].reshape(T, fin.shape[-1])
    for cp in sends:
        cp.wait_send()


def fused_body(R, Y, C, width, tokens, pre_gain, post_gain, gate_weight, up_weight, down_weight):
    L = pre_gain.shape[0]
    T, d = tokens.shape
    f = gate_weight.shape[2]
    NB = f // LANES
    Z = R // Y
    tz, ty, tc = T // R, T // Y, T // C
    G = min(CHUNKS, NB)
    groups, at = [], 0
    for g in range(G):
        nb = NB // G + (1 if g < NB % G else 0)
        groups.append((at, nb))
        at += nb
    dma = pltpu.SemaphoreType.DMA
    vm = pl.BlockSpec(memory_space=pltpu.VMEM)
    hbm = pl.BlockSpec(memory_space=pl.ANY)
    scratch = [
        pltpu.VMEM((L, d, f), BF16),
        pltpu.VMEM((L, d, f), BF16),
        pltpu.VMEM((L, f, d), BF16),
        pltpu.VMEM((L, C, tc, d), BF16),
        pltpu.VMEM((C, tc, LANES), F32),
        pltpu.VMEM((L + 1, 8, LANES), F32),
        pltpu.VMEM((L + 1, R - 1, 8, LANES), F32),
        pltpu.VMEM((L, Y - 1, NB, ty, 2 * LANES), BF16),
        pltpu.VMEM((L, Y - 1, NB, ty, 2 * LANES), BF16),
        pltpu.VMEM((NB, ty, 2 * LANES), F32),
        pltpu.VMEM((L, Z, NB, tz, 2 * LANES), BF16),
        pltpu.VMEM((L, Z - 1, NB, tz, 2 * LANES), BF16),
        pltpu.VMEM((L, Y, Z, NB, tz, LANES), BF16),
        pltpu.VMEM((L, C, tc, d), F32),
        pltpu.VMEM((L, C - 1, tc, d), F32),
        pltpu.VMEM((C, tc, d), BF16),
        dma((L, 3)),
        dma((L + 1, R - 1)), dma((L + 1, R - 1)),
        dma((L, G, Y - 1)), dma((L, G, Y - 1)),
        dma((L, G, Z - 1)), dma((L, G, Z - 1)),
        dma((L, G, Z - 1)), dma((L, G, Z - 1)),
        dma((L, G, Z, Y - 1)), dma((L, G, Z, Y - 1)),
        dma((L, C - 1)), dma((L, C - 1)),
        dma((L, C - 1)), dma((L, C - 1)),
    ]
    return pl.pallas_call(
        functools.partial(kernel, R, Y, C, tuple(groups), width),
        out_shape=jax.ShapeDtypeStruct((T, d), BF16),
        in_specs=[vm, vm, vm, hbm, hbm, hbm],
        out_specs=vm,
        scratch_shapes=scratch,
        compiler_params=pltpu.CompilerParams(
            collective_id=0, has_side_effects=True, vmem_limit_bytes=48 * 1024 * 1024
        ),
        name="window",
    )(tokens, pre_gain, post_gain, gate_weight, up_weight, down_weight)


def solution(mesh):
    R, C = mesh.shape["ra"], mesh.shape["cb"]
    Y = max(C // 2, 1)
    if R % Y:
        Y = 1

    def body(*arrays):
        tokens, gate_weight = arrays[0], arrays[3]
        T, d = tokens.shape
        width = d * R
        f = gate_weight.shape[2]
        fits = (
            1 < Y < R and C > 1 and T <= LANES and T % (16 * R) == 0 and T % (16 * C) == 0
            and (T // Y) % (T // C) == 0 and d % LANES == 0 and f % LANES == 0
        )
        if fits:
            return fused_body(R, Y, C, width, *arrays)
        return plain_body(width, *arrays)

    in_specs = (
        P(None, "ra"),
        P(None, "ra"),
        P(None, "ra"),
        P(None, "ra", "cb"),
        P(None, "ra", "cb"),
        P(None, "cb", "ra"),
    )
    return jax.shard_map(body, mesh=mesh, in_specs=in_specs, out_specs=P(None, "ra"), check_vma=False)
```

```python
import functools

import jax
import jax.numpy as jnp
from jax import lax
from jax.experimental import pallas as pl
from jax.experimental.pallas import tpu as pltpu
from jax.sharding import PartitionSpec as P

EPS = 1e-06
RES = 0.25
LANES = 128
CHUNKS = 3
F32 = jnp.float32
BF16 = jnp.bfloat16


def plain_body(width, tokens, pre_gain, post_gain, gate_weight, up_weight, down_weight):
    stream = tokens.astype(F32)
    squares = lax.psum(jnp.sum(stream * stream, axis=1), "ra")
    for l in range(pre_gain.shape[0]):
        scale_in = lax.rsqrt(squares / width + EPS)
        normed = (stream * scale_in[:, None] * pre_gain[l]).astype(BF16)
        gate = jnp.dot(normed, gate_weight[l], preferred_element_type=F32)
        up = jnp.dot(normed, up_weight[l], preferred_element_type=F32)
        gate, up = lax.psum((gate, up), "ra")
        hidden = (jax.nn.silu(gate) * up).astype(BF16)
        branch = lax.psum(jnp.dot(hidden, down_weight[l], preferred_element_type=F32), "cb")
        gained = branch * post_gain[l]
        b_sq, g_sq, cross = lax.psum(
            (
                jnp.sum(branch * branch, axis=1),
                jnp.sum(gained * gained, axis=1),
                jnp.sum(stream * gained, axis=1),
            ),
            "ra",
        )
        scale_out = lax.rsqrt(b_sq / width + EPS)
        squares = RES * RES * squares + 2.0 * RES * scale_out * cross + scale_out * scale_out * g_sq
        stream = RES * stream + gained * scale_out[:, None]
    return stream.astype(BF16)


def kernel(
    R, Y, C, groups, width,
    tok_h, pre_h, post_h, gw_h, uw_h, dw_h, out,
    tok, pre, post, gw, uw, dw, normed, sq, st_s, st_r, y_s, y_r, own, z_s, z_r, hall, b_p, b_r, fin,
    i_sem, w_sem, st_ss, st_rs, y_ss, y_rs, z_ss, z_rs, hz_ss, hz_rs, hy_ss, hy_rs, b_ss, b_rs, n_ss, n_rs,
):
    Z = R // Y
    L = pre.shape[0]
    T = tok.shape[0]
    G = len(groups)
    tz = T // R
    ty = T // Y
    tc = T // C
    per = ty // tc
    ra = lax.axis_index("ra")
    c = lax.axis_index("cb")
    z = ra // Y
    y = lax.rem(ra, Y)

    small = []
    for k, (src, dst) in enumerate(((tok_h, tok), (pre_h, pre), (post_h, post))):
        cp = pltpu.make_async_copy(src, dst, i_sem.at[k])
        cp.start()
        small.append(cp)
    loads = []
    for l in range(L):
        for k, (src, dst) in enumerate(((gw_h, gw), (uw_h, uw), (dw_h, dw))):
            cp = pltpu.make_async_copy(src.at[l], dst.at[l], w_sem.at[l, k])
            cp.start()
            loads.append(cp)

    bar = pltpu.get_barrier_semaphore()
    for s in range(1, R):
        pl.semaphore_signal(bar, inc=1, device_id={"ra": lax.rem(ra + s, R)}, device_id_type=pl.DeviceIdType.MESH)
    for s in range(1, C):
        pl.semaphore_signal(bar, inc=1, device_id={"cb": lax.rem(c + s, C)}, device_id_type=pl.DeviceIdType.MESH)

    sends = []

    def push(src, dst, ss, rs, axis, where):
        cp = pltpu.make_async_remote_copy(
            src_ref=src, dst_ref=dst, send_sem=ss, recv_sem=rs,
            device_id={axis: where}, device_id_type=pl.DeviceIdType.MESH,
        )
        cp.start()
        sends.append(cp)
        return cp

    def z_at(s):
        return lax.rem(z + s, Z) * Y + y

    def y_at(s):
        return z * Y + lax.rem(y + s, Y)

    def share_stats(i, columns):
        rows = columns[0].shape[0]
        lane = lax.broadcasted_iota(jnp.int32, (rows, LANES), 1)
        packed = jnp.zeros((rows, LANES), F32)
        for k, col in enumerate(columns):
            packed = jnp.where(lane == k, col, packed)
        if rows < LANES:
            packed = jnp.concatenate([packed, jnp.zeros((LANES - rows, LANES), F32)], axis=0)
        st_s[i] = packed.T[:8]
        cps = [
            push(st_s.at[i], st_r.at[i, s - 1], st_ss.at[i, s - 1], st_rs.at[i, s - 1], "ra", lax.rem(ra + s, R))
            for s in range(1, R)
        ]
        total = st_s[i]
        for s, cp in enumerate(cps):
            cp.wait_recv()
            total = total + st_r[i, s]
        turned = jnp.concatenate([total, jnp.zeros((LANES - 8, LANES), F32)], axis=0).T
        return [turned[:rows, k : k + 1] for k in range(len(columns))]

    for cp in small:
        cp.wait()
    tokens = tok[...].astype(F32)
    local_sq = jnp.sum(tokens * tokens, axis=1, keepdims=True)
    pl.semaphore_wait(bar, R + C - 2)

    (squares_all,) = share_stats(0, [local_sq])
    sq[...] = jnp.broadcast_to(squares_all, (T, LANES)).reshape(C, tc, LANES)
    first = (tokens * lax.rsqrt(squares_all / width + EPS) * pre[0:1, :]).astype(BF16)
    normed[0] = first.reshape(C, tc, first.shape[1])

    squares = sq[c][:, 0:1]
    stream = tok[pl.ds(pl.multiple_of(c * tc, tc), tc), :].astype(F32)

    for l in range(L):
        loads[3 * l].wait()
        loads[3 * l + 1].wait()

        def partial(half, b0, nb):
            rows = normed[l, pl.ds(half * per, per)].reshape(ty, normed.shape[-1])
            cols = slice(b0 * LANES, (b0 + nb) * LANES)
            return (
                jnp.dot(rows, gw[l, :, cols], preferred_element_type=F32),
                jnp.dot(rows, uw[l, :, cols], preferred_element_type=F32),
            )

        y_cp, z_cp, hz_cp, hy_cp = {}, {}, {}, {}

        def stage_a(g):
            b0, nb = groups[g]
            for s in range(1, Y):
                ga, ua = partial(lax.rem(y + s, Y), b0, nb)
                for i in range(nb):
                    y_s[l, s - 1, b0 + i, :, :LANES] = ga[:, i * LANES : (i + 1) * LANES].astype(BF16)
                    y_s[l, s - 1, b0 + i, :, LANES:] = ua[:, i * LANES : (i + 1) * LANES].astype(BF16)
                y_cp[g, s] = push(
                    y_s.at[l, s - 1, pl.ds(b0, nb)], y_r.at[l, s - 1, pl.ds(b0, nb)],
                    y_ss.at[l, g, s - 1], y_rs.at[l, g, s - 1], "ra", y_at(s),
                )

        def stage_a2(g):
            b0, nb = groups[g]
            ga, ua = partial(y, b0, nb)
            for i in range(nb):
                own[b0 + i, :, :LANES] = ga[:, i * LANES : (i + 1) * LANES]
                own[b0 + i, :, LANES:] = ua[:, i * LANES : (i + 1) * LANES]

        def stage_b(g):
            b0, nb = groups[g]
            total = own[b0 : b0 + nb]
            for s in range(1, Y):
                y_cp[g, s].wait_recv()
                total = total + y_r[l, s - 1, b0 : b0 + nb].astype(F32)
            own[b0 : b0 + nb] = total
            low = total.astype(BF16)
            for q in range(Z):
                z_s[l, q, b0 : b0 + nb] = low[:, q * tz : (q + 1) * tz, :]
            for s in range(1, Z):
                z_cp[g, s] = push(
                    z_s.at[l, lax.rem(z + s, Z), pl.ds(b0, nb)], z_r.at[l, s - 1, pl.ds(b0, nb)],
                    z_ss.at[l, g, s - 1], z_rs.at[l, g, s - 1], "ra", z_at(s),
                )

        def stage_c(g):
            b0, nb = groups[g]
            total = own[b0 : b0 + nb, pl.ds(pl.multiple_of(z * tz, tz), tz), :]
            for s in range(1, Z):
                z_cp[g, s].wait_recv()
                total = total + z_r[l, s - 1, b0 : b0 + nb].astype(F32)
            gate, up = total[:, :, :LANES], total[:, :, LANES:]
            hall[l, y, z, b0 : b0 + nb] = (gate / (1.0 + jnp.exp(-gate)) * up).astype(BF16)
            mine = hall.at[l, y, z, pl.ds(b0, nb)]
            for s in range(1, Z):
                hz_cp[g, s] = push(mine, mine, hz_ss.at[l, g, s - 1], hz_rs.at[l, g, s - 1], "ra", z_at(s))
            for s in range(1, Y):
                hy_cp[g, 0, s] = push(mine, mine, hy_ss.at[l, g, 0, s - 1], hy_rs.at[l, g, 0, s - 1], "ra", y_at(s))

        def stage_d(g):
            b0, nb = groups[g]
            for r in range(1, Z):
                hz_cp[g, r].wait_recv()
                got = hall.at[l, y, lax.rem(z + Z - r, Z), pl.ds(b0, nb)]
                for s in range(1, Y):
                    hy_cp[g, r, s] = push(got, got, hy_ss.at[l, g, r, s - 1], hy_rs.at[l, g, r, s - 1], "ra", y_at(s))

        def stage_e(g, acc):
            b0, nb = groups[g]
            for r in range(Z):
                for s in range(1, Y):
                    hy_cp[g, r, s].wait_recv()
            lhs = jnp.concatenate([hall[l, :, :, b0 + i].reshape(T, LANES) for i in range(nb)], axis=1)
            part = jnp.dot(lhs, dw[l, b0 * LANES : (b0 + nb) * LANES, :], preferred_element_type=F32)
            return part if acc is None else acc + part

        for g in range(G):
            stage_a(g)
        for g in range(G):
            stage_a2(g)
        acc = None
        for t in range(G + 3):
            if t < G:
                stage_b(t)
            if 0 <= t - 1 < G:
                stage_c(t - 1)
            if 0 <= t - 2 < G:
                stage_d(t - 2)
            if 0 <= t - 3 < G:
                if t == 3:
                    loads[3 * l + 2].wait()
                acc = stage_e(t - 3, acc)

        b_p[l] = acc.reshape(C, tc, acc.shape[1])
        cps = []
        for s in range(1, C):
            to = lax.rem(c + s, C)
            cps.append(push(b_p.at[l, to], b_r.at[l, s - 1], b_ss.at[l, s - 1], b_rs.at[l, s - 1], "cb", to))
        branch = b_p[l, c]
        for s, cp in enumerate(cps):
            cp.wait_recv()
            branch = branch + b_r[l, s]

        gained = branch * post[l : l + 1, :]
        b_sq, g_sq, cross = share_stats(
            l + 1,
            [
                jnp.sum(branch * branch, axis=1, keepdims=True),
                jnp.sum(gained * gained, axis=1, keepdims=True),
                jnp.sum(stream * gained, axis=1, keepdims=True),
            ],
        )
        scale_out = lax.rsqrt(b_sq / width + EPS)
        squares = RES * RES * squares + 2.0 * RES * scale_out * cross + scale_out * scale_out * g_sq
        stream = RES * stream + gained * scale_out
        if l + 1 < L:
            scale_in = lax.rsqrt(squares / width + EPS)
            normed[l + 1, c] = (stream * scale_in * pre[l + 1 : l + 2, :]).astype(BF16)
            mine = normed.at[l + 1, c]
        else:
            fin[c] = stream.astype(BF16)
            mine = fin.at[c]
        cps = [
            push(mine, mine, n_ss.at[l, s - 1], n_rs.at[l, s - 1], "cb", lax.rem(c + s, C))
            for s in range(1, C)
        ]
        for cp in cps:
            cp.wait_recv()

    out[...] = fin[...].reshape(T, fin.shape[-1])
    for cp in sends:
        cp.wait_send()


def fused_body(R, Y, C, width, tokens, pre_gain, post_gain, gate_weight, up_weight, down_weight):
    L = pre_gain.shape[0]
    T, d = tokens.shape
    f = gate_weight.shape[2]
    NB = f // LANES
    Z = R // Y
    tz, ty, tc = T // R, T // Y, T // C
    G = min(CHUNKS, NB)
    groups, at = [], 0
    for g in range(G):
        nb = NB // G + (1 if g < NB % G else 0)
        groups.append((at, nb))
        at += nb
    dma = pltpu.SemaphoreType.DMA
    vm = pl.BlockSpec(memory_space=pltpu.VMEM)
    hbm = pl.BlockSpec(memory_space=pltpu.HBM)
    scratch = [
        pltpu.VMEM((T, d), BF16),
        pltpu.VMEM((L, d), F32),
        pltpu.VMEM((L, d), F32),
        pltpu.VMEM((L, d, f), BF16),
        pltpu.VMEM((L, d, f), BF16),
        pltpu.VMEM((L, f, d), BF16),
        pltpu.VMEM((L, C, tc, d), BF16),
        pltpu.VMEM((C, tc, LANES), F32),
        pltpu.VMEM((L + 1, 8, LANES), F32),
        pltpu.VMEM((L + 1, R - 1, 8, LANES), F32),
        pltpu.VMEM((L, Y - 1, NB, ty, 2 * LANES), BF16),
        pltpu.VMEM((L, Y - 1, NB, ty, 2 * LANES), BF16),
        pltpu.VMEM((NB, ty, 2 * LANES), F32),
        pltpu.VMEM((L, Z, NB, tz, 2 * LANES), BF16),
        pltpu.VMEM((L, Z - 1, NB, tz, 2 * LANES), BF16),
        pltpu.VMEM((L, Y, Z, NB, tz, LANES), BF16),
        pltpu.VMEM((L, C, tc, d), F32),
        pltpu.VMEM((L, C - 1, tc, d), F32),
        pltpu.VMEM((C, tc, d), BF16),
        dma((3,)),
        dma((L, 3)),
        dma((L + 1, R - 1)), dma((L + 1, R - 1)),
        dma((L, G, Y - 1)), dma((L, G, Y - 1)),
        dma((L, G, Z - 1)), dma((L, G, Z - 1)),
        dma((L, G, Z - 1)), dma((L, G, Z - 1)),
        dma((L, G, Z, Y - 1)), dma((L, G, Z, Y - 1)),
        dma((L, C - 1)), dma((L, C - 1)),
        dma((L, C - 1)), dma((L, C - 1)),
    ]
    return pl.pallas_call(
        functools.partial(kernel, R, Y, C, tuple(groups), width),
        out_shape=jax.ShapeDtypeStruct((T, d), BF16),
        in_specs=[hbm] * 6,
        out_specs=vm,
        scratch_shapes=scratch,
        compiler_params=pltpu.CompilerParams(
            collective_id=0, has_side_effects=True, vmem_limit_bytes=67043328
        ),
        name="window",
    )(tokens, pre_gain, post_gain, gate_weight, up_weight, down_weight)


def solution(mesh):
    R, C = mesh.shape["ra"], mesh.shape["cb"]
    Y = max(C // 2, 1)
    if R % Y:
        Y = 1

    def body(*arrays):
        tokens, gate_weight = arrays[0], arrays[3]
        T, d = tokens.shape
        width = d * R
        f = gate_weight.shape[2]
        fits = (
            1 < Y < R and C > 1 and T <= LANES and T % (16 * R) == 0 and T % (16 * C) == 0
            and (T // Y) % (T // C) == 0 and d % LANES == 0 and f % LANES == 0
        )
        if fits:
            return fused_body(R, Y, C, width, *arrays)
        return plain_body(width, *arrays)

    in_specs = (
        P(None, "ra"),
        P(None, "ra"),
        P(None, "ra"),
        P(None, "ra", "cb"),
        P(None, "ra", "cb"),
        P(None, "cb", "ra"),
    )
    return jax.shard_map(body, mesh=mesh, in_specs=in_specs, out_specs=P(None, "ra"), check_vma=False)
```

```python
import functools

import jax
import jax.numpy as jnp
from jax import lax
from jax.experimental import pallas as pl
from jax.experimental.pallas import tpu as pltpu
from jax.sharding import PartitionSpec as P

EPS = 1e-06
RES = 0.25
LANES = 128
F32 = jnp.float32
BF16 = jnp.bfloat16


def plain_body(width, tokens, pre_gain, post_gain, gate_weight, up_weight, down_weight):
    stream = tokens.astype(F32)
    squares = lax.psum(jnp.sum(stream * stream, axis=1), "ra")
    for l in range(pre_gain.shape[0]):
        scale_in = lax.rsqrt(squares / width + EPS)
        normed = (stream * scale_in[:, None] * pre_gain[l]).astype(BF16)
        gate = jnp.dot(normed, gate_weight[l], preferred_element_type=F32)
        up = jnp.dot(normed, up_weight[l], preferred_element_type=F32)
        gate, up = lax.psum((gate, up), "ra")
        hidden = (jax.nn.silu(gate) * up).astype(BF16)
        branch = lax.psum(jnp.dot(hidden, down_weight[l], preferred_element_type=F32), "cb")
        gained = branch * post_gain[l]
        b_sq, g_sq, cross = lax.psum(
            (
                jnp.sum(branch * branch, axis=1),
                jnp.sum(gained * gained, axis=1),
                jnp.sum(stream * gained, axis=1),
            ),
            "ra",
        )
        scale_out = lax.rsqrt(b_sq / width + EPS)
        squares = RES * RES * squares + 2.0 * RES * scale_out * cross + scale_out * scale_out * g_sq
        stream = RES * stream + gained * scale_out[:, None]
    return stream.astype(BF16)


def kernel(
    R, Y, C, groups, width,
    tok_h, pre_h, post_h, gw_h, uw_h, dw_h, out,
    tok, pre, post, gw, uw, dw, normed, sq, st_s, st_r, y_s, y_r, own, z_s, z_r, hall, b_p, b_r, fin,
    i_sem, w_sem, st_ss, st_rs, y_ss, y_rs, z_ss, z_rs, hz_ss, hz_rs, hy_ss, hy_rs, b_ss, b_rs, n_ss, n_rs,
):
    Z = R // Y
    L = pre.shape[0]
    T = tok.shape[0]
    G = len(groups)
    tz = T // R
    ty = T // Y
    tc = T // C
    per = ty // tc
    ra = lax.axis_index("ra")
    c = lax.axis_index("cb")
    z = ra // Y
    y = lax.rem(ra, Y)

    small = []
    for k, (src, dst) in enumerate(((tok_h, tok), (pre_h, pre), (post_h, post))):
        cp = pltpu.make_async_copy(src, dst, i_sem.at[k])
        cp.start()
        small.append(cp)
    loads = []
    for l in range(L):
        for k, (src, dst) in enumerate(((gw_h, gw), (uw_h, uw), (dw_h, dw))):
            cp = pltpu.make_async_copy(src.at[l], dst.at[l], w_sem.at[l, k])
            cp.start()
            loads.append(cp)

    bar = pltpu.get_barrier_semaphore()
    for s in range(1, R):
        pl.semaphore_signal(bar, inc=1, device_id={"ra": lax.rem(ra + s, R)}, device_id_type=pl.DeviceIdType.MESH)
    for s in range(1, C):
        pl.semaphore_signal(bar, inc=1, device_id={"cb": lax.rem(c + s, C)}, device_id_type=pl.DeviceIdType.MESH)

    sends = []

    def push(src, dst, ss, rs, axis, where):
        cp = pltpu.make_async_remote_copy(
            src_ref=src, dst_ref=dst, send_sem=ss, recv_sem=rs,
            device_id={axis: where}, device_id_type=pl.DeviceIdType.MESH,
        )
        cp.start()
        sends.append(cp)
        return cp

    def z_at(s):
        return lax.rem(z + s, Z) * Y + y

    def y_at(s):
        return z * Y + lax.rem(y + s, Y)

    def share_stats(i, columns):
        rows = columns[0].shape[0]
        lane = lax.broadcasted_iota(jnp.int32, (rows, LANES), 1)
        packed = jnp.zeros((rows, LANES), F32)
        for k, col in enumerate(columns):
            packed = jnp.where(lane == k, col, packed)
        if rows < LANES:
            packed = jnp.concatenate([packed, jnp.zeros((LANES - rows, LANES), F32)], axis=0)
        st_s[i] = packed.T[:8]
        cps = [
            push(st_s.at[i], st_r.at[i, s - 1], st_ss.at[i, s - 1], st_rs.at[i, s - 1], "ra", lax.rem(ra + s, R))
            for s in range(1, R)
        ]
        total = st_s[i]
        for s, cp in enumerate(cps):
            cp.wait_recv()
            total = total + st_r[i, s]
        turned = jnp.concatenate([total, jnp.zeros((LANES - 8, LANES), F32)], axis=0).T
        return [turned[:rows, k : k + 1] for k in range(len(columns))]

    for cp in small:
        cp.wait()
    tokens = tok[...].astype(F32)
    local_sq = jnp.sum(tokens * tokens, axis=1, keepdims=True)
    pl.semaphore_wait(bar, R + C - 2)

    (squares_all,) = share_stats(0, [local_sq])
    sq[...] = jnp.broadcast_to(squares_all, (T, LANES)).reshape(C, tc, LANES)
    first = (tokens * lax.rsqrt(squares_all / width + EPS) * pre[0:1, :]).astype(BF16)
    normed[0] = first.reshape(C, tc, first.shape[1])

    squares = sq[c][:, 0:1]
    stream = tok[pl.ds(pl.multiple_of(c * tc, tc), tc), :].astype(F32)

    for l in range(L):
        loads[3 * l].wait()
        loads[3 * l + 1].wait()

        def partial(half, b0, nb):
            rows = normed[l, pl.ds(half * per, per)].reshape(ty, normed.shape[-1])
            cols = slice(b0 * LANES, (b0 + nb) * LANES)
            return (
                jnp.dot(rows, gw[l, :, cols], preferred_element_type=F32),
                jnp.dot(rows, uw[l, :, cols], preferred_element_type=F32),
            )

        y_cp, z_cp, hz_cp, hy_cp = {}, {}, {}, {}

        def stage_a(g):
            b0, nb = groups[g]
            for s in range(1, Y):
                ga, ua = partial(lax.rem(y + s, Y), b0, nb)
                for i in range(nb):
                    y_s[l, s - 1, b0 + i, :, :LANES] = ga[:, i * LANES : (i + 1) * LANES].astype(BF16)
                    y_s[l, s - 1, b0 + i, :, LANES:] = ua[:, i * LANES : (i + 1) * LANES].astype(BF16)
                y_cp[g, s] = push(
                    y_s.at[l, s - 1, pl.ds(b0, nb)], y_r.at[l, s - 1, pl.ds(b0, nb)],
                    y_ss.at[l, g, s - 1], y_rs.at[l, g, s - 1], "ra", y_at(s),
                )

        def stage_a2(g):
            b0, nb = groups[g]
            ga, ua = partial(y, b0, nb)
            for i in range(nb):
                own[b0 + i, :, :LANES] = ga[:, i * LANES : (i + 1) * LANES]
                own[b0 + i, :, LANES:] = ua[:, i * LANES : (i + 1) * LANES]

        def stage_b(g):
            b0, nb = groups[g]
            total = own[b0 : b0 + nb]
            for s in range(1, Y):
                y_cp[g, s].wait_recv()
                total = total + y_r[l, s - 1, b0 : b0 + nb].astype(F32)
            own[b0 : b0 + nb] = total
            low = total.astype(BF16)
            for q in range(Z):
                z_s[l, q, b0 : b0 + nb] = low[:, q * tz : (q + 1) * tz, :]
            for s in range(1, Z):
                z_cp[g, s] = push(
                    z_s.at[l, lax.rem(z + s, Z), pl.ds(b0, nb)], z_r.at[l, s - 1, pl.ds(b0, nb)],
                    z_ss.at[l, g, s - 1], z_rs.at[l, g, s - 1], "ra", z_at(s),
                )

        def stage_c(g):
            b0, nb = groups[g]
            total = own[b0 : b0 + nb, pl.ds(pl.multiple_of(z * tz, tz), tz), :]
            for s in range(1, Z):
                z_cp[g, s].wait_recv()
                total = total + z_r[l, s - 1, b0 : b0 + nb].astype(F32)
            gate, up = total[:, :, :LANES], total[:, :, LANES:]
            hall[l, y, z, b0 : b0 + nb] = (gate / (1.0 + jnp.exp(-gate)) * up).astype(BF16)
            mine = hall.at[l, y, z, pl.ds(b0, nb)]
            for s in range(1, Z):
                hz_cp[g, s] = push(mine, mine, hz_ss.at[l, g, s - 1], hz_rs.at[l, g, s - 1], "ra", z_at(s))
            for s in range(1, Y):
                hy_cp[g, 0, s] = push(mine, mine, hy_ss.at[l, g, 0, s - 1], hy_rs.at[l, g, 0, s - 1], "ra", y_at(s))

        def stage_d(g):
            b0, nb = groups[g]
            for r in range(1, Z):
                hz_cp[g, r].wait_recv()
                got = hall.at[l, y, lax.rem(z + Z - r, Z), pl.ds(b0, nb)]
                for s in range(1, Y):
                    hy_cp[g, r, s] = push(got, got, hy_ss.at[l, g, r, s - 1], hy_rs.at[l, g, r, s - 1], "ra", y_at(s))

        def stage_e(g, acc):
            b0, nb = groups[g]
            for r in range(Z):
                for s in range(1, Y):
                    hy_cp[g, r, s].wait_recv()
            lhs = jnp.concatenate([hall[l, :, :, b0 + i].reshape(T, LANES) for i in range(nb)], axis=1)
            part = jnp.dot(lhs, dw[l, b0 * LANES : (b0 + nb) * LANES, :], preferred_element_type=F32)
            return part if acc is None else acc + part

        for g in range(G):
            stage_a(g)
        for g in range(G):
            stage_a2(g)
        acc = None
        for t in range(G + 3):
            if t < G:
                stage_b(t)
            if 0 <= t - 1 < G:
                stage_c(t - 1)
            if 0 <= t - 2 < G:
                stage_d(t - 2)
            if 0 <= t - 3 < G:
                if t == 3:
                    loads[3 * l + 2].wait()
                acc = stage_e(t - 3, acc)

        b_p[l] = acc.reshape(C, tc, acc.shape[1])
        cps = []
        for s in range(1, C):
            to = lax.rem(c + s, C)
            cps.append(push(b_p.at[l, to], b_r.at[l, s - 1], b_ss.at[l, s - 1], b_rs.at[l, s - 1], "cb", to))
        branch = b_p[l, c]
        for s, cp in enumerate(cps):
            cp.wait_recv()
            branch = branch + b_r[l, s]

        gained = branch * post[l : l + 1, :]
        b_sq, g_sq, cross = share_stats(
            l + 1,
            [
                jnp.sum(branch * branch, axis=1, keepdims=True),
                jnp.sum(gained * gained, axis=1, keepdims=True),
                jnp.sum(stream * gained, axis=1, keepdims=True),
            ],
        )
        scale_out = lax.rsqrt(b_sq / width + EPS)
        squares = RES * RES * squares + 2.0 * RES * scale_out * cross + scale_out * scale_out * g_sq
        stream = RES * stream + gained * scale_out
        if l + 1 < L:
            scale_in = lax.rsqrt(squares / width + EPS)
            normed[l + 1, c] = (stream * scale_in * pre[l + 1 : l + 2, :]).astype(BF16)
            mine = normed.at[l + 1, c]
        else:
            fin[c] = stream.astype(BF16)
            mine = fin.at[c]
        cps = [
            push(mine, mine, n_ss.at[l, s - 1], n_rs.at[l, s - 1], "cb", lax.rem(c + s, C))
            for s in range(1, C)
        ]
        for cp in cps:
            cp.wait_recv()

    out[...] = fin[...].reshape(T, fin.shape[-1])
    for cp in sends:
        cp.wait_send()


def fused_body(R, Y, C, width, tokens, pre_gain, post_gain, gate_weight, up_weight, down_weight):
    L = pre_gain.shape[0]
    T, d = tokens.shape
    f = gate_weight.shape[2]
    NB = f // LANES
    Z = R // Y
    tz, ty, tc = T // R, T // Y, T // C
    head = max(NB // 5, 1) if NB > 2 else 0
    rest = NB - head
    sizes = [n for n in (head, rest - rest // 2, rest // 2) if n]
    G = len(sizes)
    groups, at = [], 0
    for nb in sizes:
        groups.append((at, nb))
        at += nb
    dma = pltpu.SemaphoreType.DMA
    vm = pl.BlockSpec(memory_space=pltpu.VMEM)
    hbm = pl.BlockSpec(memory_space=pltpu.HBM)
    scratch = [
        pltpu.VMEM((T, d), BF16),
        pltpu.VMEM((L, d), F32),
        pltpu.VMEM((L, d), F32),
        pltpu.VMEM((L, d, f), BF16),
        pltpu.VMEM((L, d, f), BF16),
        pltpu.VMEM((L, f, d), BF16),
        pltpu.VMEM((L, C, tc, d), BF16),
        pltpu.VMEM((C, tc, LANES), F32),
        pltpu.VMEM((L + 1, 8, LANES), F32),
        pltpu.VMEM((L + 1, R - 1, 8, LANES), F32),
        pltpu.VMEM((L, Y - 1, NB, ty, 2 * LANES), BF16),
        pltpu.VMEM((L, Y - 1, NB, ty, 2 * LANES), BF16),
        pltpu.VMEM((NB, ty, 2 * LANES), F32),
        pltpu.VMEM((L, Z, NB, tz, 2 * LANES), BF16),
        pltpu.VMEM((L, Z - 1, NB, tz, 2 * LANES), BF16),
        pltpu.VMEM((L, Y, Z, NB, tz, LANES), BF16),
        pltpu.VMEM((L, C, tc, d), F32),
        pltpu.VMEM((L, C - 1, tc, d), F32),
        pltpu.VMEM((C, tc, d), BF16),
        dma((3,)),
        dma((L, 3)),
        dma((L + 1, R - 1)), dma((L + 1, R - 1)),
        dma((L, G, Y - 1)), dma((L, G, Y - 1)),
        dma((L, G, Z - 1)), dma((L, G, Z - 1)),
        dma((L, G, Z - 1)), dma((L, G, Z - 1)),
        dma((L, G, Z, Y - 1)), dma((L, G, Z, Y - 1)),
        dma((L, C - 1)), dma((L, C - 1)),
        dma((L, C - 1)), dma((L, C - 1)),
    ]
    return pl.pallas_call(
        functools.partial(kernel, R, Y, C, tuple(groups), width),
        out_shape=jax.ShapeDtypeStruct((T, d), BF16),
        in_specs=[hbm] * 6,
        out_specs=vm,
        scratch_shapes=scratch,
        compiler_params=pltpu.CompilerParams(
            collective_id=0, has_side_effects=True, vmem_limit_bytes=67043328
        ),
        name="window",
    )(tokens, pre_gain, post_gain, gate_weight, up_weight, down_weight)


def solution(mesh):
    R, C = mesh.shape["ra"], mesh.shape["cb"]
    Y = max(C // 2, 1)
    if R % Y:
        Y = 1

    def body(*arrays):
        tokens, gate_weight = arrays[0], arrays[3]
        T, d = tokens.shape
        width = d * R
        f = gate_weight.shape[2]
        fits = (
            1 < Y < R and C > 1 and T <= LANES and T % (16 * R) == 0 and T % (16 * C) == 0
            and (T // Y) % (T // C) == 0 and d % LANES == 0 and f % LANES == 0
        )
        if fits:
            return fused_body(R, Y, C, width, *arrays)
        return plain_body(width, *arrays)

    in_specs = (
        P(None, "ra"),
        P(None, "ra"),
        P(None, "ra"),
        P(None, "ra", "cb"),
        P(None, "ra", "cb"),
        P(None, "cb", "ra"),
    )
    return jax.shard_map(body, mesh=mesh, in_specs=in_specs, out_specs=P(None, "ra"), check_vma=False)
```

```python
import functools

import jax
import jax.numpy as jnp
from jax import lax
from jax.experimental import pallas as pl
from jax.experimental.pallas import tpu as pltpu
from jax.sharding import PartitionSpec as P

EPS = 1e-06
RES = 0.25
LANES = 128
F32 = jnp.float32
BF16 = jnp.bfloat16


def plain_body(width, tokens, pre_gain, post_gain, gate_weight, up_weight, down_weight):
    stream = tokens.astype(F32)
    squares = lax.psum(jnp.sum(stream * stream, axis=1), "ra")
    for l in range(pre_gain.shape[0]):
        scale_in = lax.rsqrt(squares / width + EPS)
        normed = (stream * scale_in[:, None] * pre_gain[l]).astype(BF16)
        gate = jnp.dot(normed, gate_weight[l], preferred_element_type=F32)
        up = jnp.dot(normed, up_weight[l], preferred_element_type=F32)
        gate, up = lax.psum((gate, up), "ra")
        hidden = (jax.nn.silu(gate) * up).astype(BF16)
        branch = lax.psum(jnp.dot(hidden, down_weight[l], preferred_element_type=F32), "cb")
        gained = branch * post_gain[l]
        b_sq, g_sq, cross = lax.psum(
            (
                jnp.sum(branch * branch, axis=1),
                jnp.sum(gained * gained, axis=1),
                jnp.sum(stream * gained, axis=1),
            ),
            "ra",
        )
        scale_out = lax.rsqrt(b_sq / width + EPS)
        squares = RES * RES * squares + 2.0 * RES * scale_out * cross + scale_out * scale_out * g_sq
        stream = RES * stream + gained * scale_out[:, None]
    return stream.astype(BF16)


def kernel(
    R, Y, C, groups, width,
    tok_h, pre_h, post_h, gw_h, uw_h, dw_h, out,
    tok, pre, post, gw, uw, dw, normed, sq, st_s, st_r, y_s, y_r, own, z_s, z_r, hall, b_p, b_r, fin,
    i_sem, w_sem, st_ss, st_rs, y_ss, y_rs, z_ss, z_rs, hz_ss, hz_rs, hy_ss, hy_rs, b_ss, b_rs, n_ss, n_rs,
):
    Z = R // Y
    L = pre.shape[0]
    T = tok.shape[0]
    G = len(groups)
    tz = T // R
    ty = T // Y
    tc = T // C
    per = ty // tc
    ra = lax.axis_index("ra")
    c = lax.axis_index("cb")
    z = ra // Y
    y = lax.rem(ra, Y)

    small = []
    for k, (src, dst) in enumerate(((tok_h, tok), (pre_h, pre), (post_h, post))):
        cp = pltpu.make_async_copy(src, dst, i_sem.at[k])
        cp.start()
        small.append(cp)
    loads = []
    for l in range(L):
        for k, (src, dst) in enumerate(((gw_h, gw), (uw_h, uw), (dw_h, dw))):
            cp = pltpu.make_async_copy(src.at[l], dst.at[l], w_sem.at[l, k])
            cp.start()
            loads.append(cp)

    bar = pltpu.get_barrier_semaphore()
    for s in range(1, R):
        pl.semaphore_signal(bar, inc=1, device_id={"ra": lax.rem(ra + s, R)}, device_id_type=pl.DeviceIdType.MESH)
    for s in range(1, C):
        pl.semaphore_signal(bar, inc=1, device_id={"cb": lax.rem(c + s, C)}, device_id_type=pl.DeviceIdType.MESH)

    sends = []

    def push(src, dst, ss, rs, axis, where):
        cp = pltpu.make_async_remote_copy(
            src_ref=src, dst_ref=dst, send_sem=ss, recv_sem=rs,
            device_id={axis: where}, device_id_type=pl.DeviceIdType.MESH,
        )
        cp.start()
        sends.append(cp)
        return cp

    def z_at(s):
        return lax.rem(z + s, Z) * Y + y

    def y_at(s):
        return z * Y + lax.rem(y + s, Y)

    def share_stats(i, columns):
        rows = columns[0].shape[0]
        lane = lax.broadcasted_iota(jnp.int32, (rows, LANES), 1)
        packed = jnp.zeros((rows, LANES), F32)
        for k, col in enumerate(columns):
            packed = jnp.where(lane == k, col, packed)
        if rows < LANES:
            packed = jnp.concatenate([packed, jnp.zeros((LANES - rows, LANES), F32)], axis=0)
        st_s[i] = packed.T[:8]
        cps = [
            push(st_s.at[i], st_r.at[i, s - 1], st_ss.at[i, s - 1], st_rs.at[i, s - 1], "ra", lax.rem(ra + s, R))
            for s in range(1, R)
        ]
        total = st_s[i]
        for s, cp in enumerate(cps):
            cp.wait_recv()
            total = total + st_r[i, s]
        turned = jnp.concatenate([total, jnp.zeros((LANES - 8, LANES), F32)], axis=0).T
        return [turned[:rows, k : k + 1] for k in range(len(columns))]

    for cp in small:
        cp.wait()
    tokens = tok[...].astype(F32)
    local_sq = jnp.sum(tokens * tokens, axis=1, keepdims=True)
    pl.semaphore_wait(bar, R + C - 2)

    (squares_all,) = share_stats(0, [local_sq])
    sq[...] = jnp.broadcast_to(squares_all, (T, LANES)).reshape(C, tc, LANES)
    first = (tokens * lax.rsqrt(squares_all / width + EPS) * pre[0:1, :]).astype(BF16)
    normed[0] = first.reshape(C, tc, first.shape[1])

    squares = sq[c][:, 0:1]
    stream = tok[pl.ds(pl.multiple_of(c * tc, tc), tc), :].astype(F32)

    for l in range(L):
        loads[3 * l].wait()
        loads[3 * l + 1].wait()

        def partial(half, b0, nb):
            rows = normed[l, pl.ds(half * per, per)].reshape(ty, normed.shape[-1])
            cols = slice(b0 * LANES, (b0 + nb) * LANES)
            return (
                jnp.dot(rows, gw[l, :, cols], preferred_element_type=F32),
                jnp.dot(rows, uw[l, :, cols], preferred_element_type=F32),
            )

        y_cp, z_cp, hz_cp, hy_cp = {}, {}, {}, {}

        def stage_a(g):
            b0, nb = groups[g]
            for s in range(1, Y):
                ga, ua = partial(lax.rem(y + s, Y), b0, nb)
                for i in range(nb):
                    y_s[l, s - 1, b0 + i, :, :LANES] = ga[:, i * LANES : (i + 1) * LANES].astype(BF16)
                    y_s[l, s - 1, b0 + i, :, LANES:] = ua[:, i * LANES : (i + 1) * LANES].astype(BF16)
                y_cp[g, s] = push(
                    y_s.at[l, s - 1, pl.ds(b0, nb)], y_r.at[l, s - 1, pl.ds(b0, nb)],
                    y_ss.at[l, g, s - 1], y_rs.at[l, g, s - 1], "ra", y_at(s),
                )

        def stage_a2(g):
            b0, nb = groups[g]
            ga, ua = partial(y, b0, nb)
            for i in range(nb):
                own[b0 + i, :, :LANES] = ga[:, i * LANES : (i + 1) * LANES]
                own[b0 + i, :, LANES:] = ua[:, i * LANES : (i + 1) * LANES]

        def stage_b(g):
            b0, nb = groups[g]
            total = own[b0 : b0 + nb]
            for s in range(1, Y):
                y_cp[g, s].wait_recv()
                total = total + y_r[l, s - 1, b0 : b0 + nb].astype(F32)
            own[b0 : b0 + nb] = total
            low = total.astype(BF16)
            for q in range(Z):
                z_s[l, q, b0 : b0 + nb] = low[:, q * tz : (q + 1) * tz, :]
            for s in range(1, Z):
                z_cp[g, s] = push(
                    z_s.at[l, lax.rem(z + s, Z), pl.ds(b0, nb)], z_r.at[l, s - 1, pl.ds(b0, nb)],
                    z_ss.at[l, g, s - 1], z_rs.at[l, g, s - 1], "ra", z_at(s),
                )

        def stage_c(g):
            b0, nb = groups[g]
            total = own[b0 : b0 + nb, pl.ds(pl.multiple_of(z * tz, tz), tz), :]
            for s in range(1, Z):
                z_cp[g, s].wait_recv()
                total = total + z_r[l, s - 1, b0 : b0 + nb].astype(F32)
            gate, up = total[:, :, :LANES], total[:, :, LANES:]
            hall[l, y, z, b0 : b0 + nb] = (gate / (1.0 + jnp.exp(-gate)) * up).astype(BF16)
            mine = hall.at[l, y, z, pl.ds(b0, nb)]
            for s in range(1, Z):
                hz_cp[g, s] = push(mine, mine, hz_ss.at[l, g, s - 1], hz_rs.at[l, g, s - 1], "ra", z_at(s))
            for s in range(1, Y):
                hy_cp[g, 0, s] = push(mine, mine, hy_ss.at[l, g, 0, s - 1], hy_rs.at[l, g, 0, s - 1], "ra", y_at(s))

        def stage_d(g):
            b0, nb = groups[g]
            for r in range(1, Z):
                hz_cp[g, r].wait_recv()
                got = hall.at[l, y, lax.rem(z + Z - r, Z), pl.ds(b0, nb)]
                for s in range(1, Y):
                    hy_cp[g, r, s] = push(got, got, hy_ss.at[l, g, r, s - 1], hy_rs.at[l, g, r, s - 1], "ra", y_at(s))

        def stage_e(g, acc):
            b0, nb = groups[g]
            for r in range(Z):
                for s in range(1, Y):
                    hy_cp[g, r, s].wait_recv()
            lhs = jnp.concatenate([hall[l, :, :, b0 + i].reshape(T, LANES) for i in range(nb)], axis=1)
            part = jnp.dot(lhs, dw[l, b0 * LANES : (b0 + nb) * LANES, :], preferred_element_type=F32)
            return part if acc is None else acc + part

        for g in range(G):
            stage_a(g)
        stage_a2(0)
        acc = None
        for t in range(G + 3):
            if t < G:
                stage_b(t)
                if t + 1 < G:
                    stage_a2(t + 1)
            if 0 <= t - 1 < G:
                stage_c(t - 1)
            if 0 <= t - 2 < G:
                stage_d(t - 2)
            if 0 <= t - 3 < G:
                if t == 3:
                    loads[3 * l + 2].wait()
                acc = stage_e(t - 3, acc)

        b_p[l] = acc.reshape(C, tc, acc.shape[1])
        cps = []
        for s in range(1, C):
            to = lax.rem(c + s, C)
            cps.append(push(b_p.at[l, to], b_r.at[l, s - 1], b_ss.at[l, s - 1], b_rs.at[l, s - 1], "cb", to))
        branch = b_p[l, c]
        for s, cp in enumerate(cps):
            cp.wait_recv()
            branch = branch + b_r[l, s]

        gained = branch * post[l : l + 1, :]
        b_sq, g_sq, cross = share_stats(
            l + 1,
            [
                jnp.sum(branch * branch, axis=1, keepdims=True),
                jnp.sum(gained * gained, axis=1, keepdims=True),
                jnp.sum(stream * gained, axis=1, keepdims=True),
            ],
        )
        scale_out = lax.rsqrt(b_sq / width + EPS)
        squares = RES * RES * squares + 2.0 * RES * scale_out * cross + scale_out * scale_out * g_sq
        stream = RES * stream + gained * scale_out
        if l + 1 < L:
            scale_in = lax.rsqrt(squares / width + EPS)
            normed[l + 1, c] = (stream * scale_in * pre[l + 1 : l + 2, :]).astype(BF16)
            mine = normed.at[l + 1, c]
        else:
            fin[c] = stream.astype(BF16)
            mine = fin.at[c]
        cps = [
            push(mine, mine, n_ss.at[l, s - 1], n_rs.at[l, s - 1], "cb", lax.rem(c + s, C))
            for s in range(1, C)
        ]
        for cp in cps:
            cp.wait_recv()

    out[...] = fin[...].reshape(T, fin.shape[-1])
    for cp in sends:
        cp.wait_send()


def fused_body(R, Y, C, width, tokens, pre_gain, post_gain, gate_weight, up_weight, down_weight):
    L = pre_gain.shape[0]
    T, d = tokens.shape
    f = gate_weight.shape[2]
    NB = f // LANES
    Z = R // Y
    tz, ty, tc = T // R, T // Y, T // C
    head = max(NB // 5, 1) if NB > 2 else 0
    rest = NB - head
    sizes = [n for n in (head, rest - rest // 2, rest // 2) if n]
    G = len(sizes)
    groups, at = [], 0
    for nb in sizes:
        groups.append((at, nb))
        at += nb
    dma = pltpu.SemaphoreType.DMA
    vm = pl.BlockSpec(memory_space=pltpu.VMEM)
    hbm = pl.BlockSpec(memory_space=pltpu.HBM)
    scratch = [
        pltpu.VMEM((T, d), BF16),
        pltpu.VMEM((L, d), F32),
        pltpu.VMEM((L, d), F32),
        pltpu.VMEM((L, d, f), BF16),
        pltpu.VMEM((L, d, f), BF16),
        pltpu.VMEM((L, f, d), BF16),
        pltpu.VMEM((L, C, tc, d), BF16),
        pltpu.VMEM((C, tc, LANES), F32),
        pltpu.VMEM((L + 1, 8, LANES), F32),
        pltpu.VMEM((L + 1, R - 1, 8, LANES), F32),
        pltpu.VMEM((L, Y - 1, NB, ty, 2 * LANES), BF16),
        pltpu.VMEM((L, Y - 1, NB, ty, 2 * LANES), BF16),
        pltpu.VMEM((NB, ty, 2 * LANES), F32),
        pltpu.VMEM((L, Z, NB, tz, 2 * LANES), BF16),
        pltpu.VMEM((L, Z - 1, NB, tz, 2 * LANES), BF16),
        pltpu.VMEM((L, Y, Z, NB, tz, LANES), BF16),
        pltpu.VMEM((L, C, tc, d), F32),
        pltpu.VMEM((L, C - 1, tc, d), F32),
        pltpu.VMEM((C, tc, d), BF16),
        dma((3,)),
        dma((L, 3)),
        dma((L + 1, R - 1)), dma((L + 1, R - 1)),
        dma((L, G, Y - 1)), dma((L, G, Y - 1)),
        dma((L, G, Z - 1)), dma((L, G, Z - 1)),
        dma((L, G, Z - 1)), dma((L, G, Z - 1)),
        dma((L, G, Z, Y - 1)), dma((L, G, Z, Y - 1)),
        dma((L, C - 1)), dma((L, C - 1)),
        dma((L, C - 1)), dma((L, C - 1)),
    ]
    return pl.pallas_call(
        functools.partial(kernel, R, Y, C, tuple(groups), width),
        out_shape=jax.ShapeDtypeStruct((T, d), BF16),
        in_specs=[hbm] * 6,
        out_specs=vm,
        scratch_shapes=scratch,
        compiler_params=pltpu.CompilerParams(
            collective_id=0, has_side_effects=True, vmem_limit_bytes=67043328
        ),
        name="window",
    )(tokens, pre_gain, post_gain, gate_weight, up_weight, down_weight)


def solution(mesh):
    R, C = mesh.shape["ra"], mesh.shape["cb"]
    Y = max(C // 2, 1)
    if R % Y:
        Y = 1

    def body(*arrays):
        tokens, gate_weight = arrays[0], arrays[3]
        T, d = tokens.shape
        width = d * R
        f = gate_weight.shape[2]
        fits = (
            1 < Y < R and C > 1 and T <= LANES and T % (16 * R) == 0 and T % (16 * C) == 0
            and (T // Y) % (T // C) == 0 and d % LANES == 0 and f % LANES == 0
        )
        if fits:
            return fused_body(R, Y, C, width, *arrays)
        return plain_body(width, *arrays)

    in_specs = (
        P(None, "ra"),
        P(None, "ra"),
        P(None, "ra"),
        P(None, "ra", "cb"),
        P(None, "ra", "cb"),
        P(None, "cb", "ra"),
    )
    return jax.shard_map(body, mesh=mesh, in_specs=in_specs, out_specs=P(None, "ra"), check_vma=False)
```
